32 devices in a mesh: sp: 16 (over z, y, x), tp: 2 (over core).
Axes of the slice: x: 2, y: 2, z: 4, core: 2. Of those that a mesh axis runs over, the one named last changes fastest.
Arguments:
- tokens: bfloat16 [16384, 2048], P(('sp', 'tp')), may hold values from -6 to 6
- norm_gain: float32 [2048], replicated, may hold values from 0.1 to 1.9
- w_query: bfloat16 [2048, 1024], P('sp', 'tp'), may hold values from -0.125 to 0.125
- w_key: bfloat16 [2048, 1024], P('sp', 'tp'), may hold values from -0.125 to 0.125
- w_value: bfloat16 [2048, 1024], P('sp', 'tp'), may hold values from -0.125 to 0.125
- decay_rate: float32 [128, 8], P('sp', 'tp'), may hold values from 3.0517578e-06 to 0.1, as said below
- state_init: float32 [8, 128, 128], P('tp'), may hold values from -48 to 48
- out_gain: float32 [1024], P('tp'), may hold values from 0.1 to 1.9
- w_out: bfloat16 [1024, 2048], P('tp', 'sp'), may hold values from -0.1875 to 0.1875
Outputs:
- mixed: bfloat16 [16384, 2048], P(('sp', 'tp'))
The draws below stay inside these ranges and needn't reach their ends.
Inputs may be any that keep to these rules, and one draw needn't show every extreme that they name: `decay_rate`: constant over each block of 128 positions.
All inputs are finite; a program needn't handle non-finite values.
Results may differ from the reference program's by a relative error of at most 0.025.
Values may be sent and summed in bfloat16 or wider, within the bound.
A program may use at most 64 MiB of HBM per device.

```python
import math
import jax
import jax.numpy as jnp
from jax import lax

D = 2048
HEADS = 8
HEAD_DIM = 128
BLOCK = 128
SEQ = 16384
RET_WIDTH = 1024
N_TP = 2


def draw_decay_rate(key, part):
    keys = jax.random.split(key, 4)
    count_blocks = SEQ // BLOCK
    fast_share = 0.5
    fast_heads = jax.random.uniform(keys[0], (HEADS,), jnp.float32) < fast_share
    slow_base = math.log(10.0) / SEQ * jnp.exp(jax.random.uniform(keys[1], (HEADS,), jnp.float32, math.log(0.15), math.log(0.5)))
    fast_base = jnp.exp(jax.random.uniform(keys[2], (HEADS,), jnp.float32, math.log(1.0 / 50.0), math.log(1.0 / 25.0)))
    factor = jnp.exp(jax.random.uniform(keys[3], (count_blocks, HEADS), jnp.float32, math.log(0.5), math.log(2.0)))
    return (jnp.where(fast_heads, fast_base, slow_base)[None, :] * factor).astype(jnp.float32)


def level_of(key, extent, pieces, smallest, high):
    def one(position, parts):
        draws = jax.random.uniform(jax.random.fold_in(jax.random.fold_in(key, 6), position), (parts,), jnp.float32, smallest / len(pieces), high / len(pieces))
        return jnp.repeat(jnp.exp(draws), extent[position] // parts).reshape((-1,) + (1,) * (len(extent) - position - 1))

    gain = one(*pieces[0])
    for cut in pieces[1:]:
        gain = gain * one(*cut)
    return gain


def scatter_about(key, shape, deviation, bound, cuts=(), kind=jnp.bfloat16):
    entries = jax.random.normal(key, shape, jnp.float32) * deviation
    if len(cuts) > 0:
        entries = level_of(key, shape, cuts, -0.22, 0.18) * entries
    return jnp.clip(entries, min=-bound, max=bound).astype(kind)


def setup_inputs(seed: int = 0) -> dict:
    seeds = jax.random.split(jax.random.key(seed), 10)
    tokens = scatter_about(seeds[0], (SEQ, D), 1.0, 6.0, ((0, 32),))
    norm_gain = jnp.clip(1.0 + 0.18 * jax.random.normal(seeds[1], (D,), jnp.float32), 0.1, 1.9)
    w_query = scatter_about(seeds[2], (D, RET_WIDTH), D ** -0.5, 0.125, ((0, 16), (1, 2)))
    w_key = scatter_about(seeds[3], (D, RET_WIDTH), D ** -0.5, 0.125, ((0, 16), (1, 2)))
    w_value = scatter_about(seeds[4], (D, RET_WIDTH), D ** -0.5, 0.125, ((0, 16), (1, 2)))
    decay_rate = draw_decay_rate(jax.random.fold_in(seeds[9], 71), 0)
    state_init = scatter_about(seeds[6], (HEADS, HEAD_DIM, HEAD_DIM), 8.0, 48.0, ((0, 2),), jnp.float32)
    out_gain = jnp.clip(1.0 + 0.18 * jax.random.normal(seeds[7], (RET_WIDTH,), jnp.float32), 0.1, 1.9)
    w_out = scatter_about(seeds[8], (RET_WIDTH, D), RET_WIDTH ** -0.5, 0.1875, ((0, 2), (1, 16)))
    return {"tokens": tokens, "norm_gain": norm_gain, "w_query": w_query, "w_key": w_key, "w_value": w_value, "decay_rate": decay_rate, "state_init": state_init, "out_gain": out_gain, "w_out": w_out}


EPS = 0.1
ROPE_BASE = 10000.0

def rotate(values_in, positions):
    half_dim = values_in.shape[-1] // 2
    inv_freq = ROPE_BASE ** (-jnp.arange(half_dim, dtype=jnp.float32) / half_dim)
    angles = positions[:, None] * inv_freq[None, :]
    cosine = jnp.cos(angles)[:, None, :]
    sine_part = jnp.sin(angles)[:, None, :]
    first_half = values_in[..., :half_dim]
    second_half = values_in[..., half_dim:]
    return jnp.concatenate([first_half * cosine - second_half * sine_part, second_half * cosine + first_half * sine_part], axis=-1)

def reference(tokens, norm_gain, w_query, w_key, w_value, decay_rate, state_init, out_gain, w_out):
    high = lax.Precision.HIGHEST
    values_in = tokens.astype(jnp.float32)
    normed = (values_in * lax.rsqrt(lax.optimization_barrier(jnp.mean(values_in * values_in, axis=-1, keepdims=True)) + EPS) * norm_gain).astype(jnp.bfloat16)
    positions = jnp.arange(SEQ, dtype=jnp.float32)
    query_rot = rotate(jnp.dot(normed, w_query, preferred_element_type=jnp.float32).reshape(SEQ, HEADS, HEAD_DIM), positions).astype(jnp.bfloat16)
    key_rot = rotate(jnp.dot(normed, w_key, preferred_element_type=jnp.float32).reshape(SEQ, HEADS, HEAD_DIM), positions).astype(jnp.bfloat16)
    value_rows = jnp.dot(normed, w_value, preferred_element_type=jnp.float32).astype(jnp.bfloat16)
    value_rows = value_rows.reshape(SEQ, HEADS, HEAD_DIM)
    count_blocks = SEQ // BLOCK
    q_blocks = query_rot.astype(jnp.float32).reshape(count_blocks, BLOCK, HEADS, HEAD_DIM)
    k_blocks = key_rot.astype(jnp.float32).reshape(count_blocks, BLOCK, HEADS, HEAD_DIM) * HEAD_DIM ** (-0.5)
    v_blocks = value_rows.astype(jnp.float32).reshape(count_blocks, BLOCK, HEADS, HEAD_DIM)
    offsets = jnp.arange(BLOCK, dtype=jnp.float32)
    step_gap = offsets[:, None] - offsets[None, :]

    def advance(state_now, block_item):
        q_one, k_one, v_one, rate_one = block_item
        inside = jnp.where(step_gap[None] >= 0.0, jnp.exp(-jnp.maximum(step_gap, 0.0)[None] * rate_one[:, None, None]), 0.0)
        scores = jnp.einsum('ihd,jhd->hij', q_one, k_one, precision=high) * inside
        inner_part = jnp.einsum('hij,jhe->ihe', scores, v_one, precision=high)
        read_decay = jnp.exp(-(offsets + 1.0)[:, None] * rate_one[None, :])
        cross_part = jnp.einsum('ihd,hde->ihe', q_one, state_now, precision=high) * read_decay[:, :, None]
        tail_decay = jnp.exp(-(BLOCK - 1.0 - offsets)[:, None] * rate_one[None, :])
        block_kv = jnp.einsum('jhd,jhe->hde', k_one * tail_decay[:, :, None], v_one, precision=high)
        state_next = jnp.exp(-BLOCK * rate_one)[:, None, None] * state_now + block_kv
        return (state_next, inner_part + cross_part)
    final_state, retained = lax.scan(advance, state_init.astype(jnp.float32), (q_blocks, k_blocks, v_blocks, decay_rate))
    out_heads = retained.reshape(SEQ, HEADS, HEAD_DIM)
    out_heads = out_heads * lax.rsqrt(lax.optimization_barrier(jnp.mean(out_heads * out_heads, axis=-1, keepdims=True)) + EPS)
    out_heads = out_heads * out_gain.reshape(HEADS, HEAD_DIM)
    hidden = out_heads.reshape(SEQ, RET_WIDTH).astype(jnp.bfloat16)
    group_cols = RET_WIDTH // N_TP
    total_sum = jnp.zeros((SEQ, D), jnp.float32)
    for group in range(N_TP):
        partial_value = jnp.dot(hidden[:, group * group_cols:(group + 1) * group_cols], w_out[group * group_cols:(group + 1) * group_cols], preferred_element_type=jnp.float32).astype(jnp.bfloat16)
        partial_value = lax.optimization_barrier(partial_value)
        total_sum = total_sum + partial_value.astype(jnp.float32)
    return total_sum.astype(jnp.bfloat16)
```

```python
import functools

import jax
import jax.numpy as jnp
from jax import lax
from jax.experimental import pallas as pl
from jax.experimental.pallas import tpu as pltpu
from jax.sharding import PartitionSpec as P

HEAD_DIM = 128
BLOCK = 128
EPS = 0.1
ROPE_BASE = 10000.0
MESH = pl.DeviceIdType.MESH
F32 = jnp.float32
BF16 = jnp.bfloat16


def remote(src, dst, send, recv, device):
    return pltpu.make_async_remote_copy(
        src_ref=src, dst_ref=dst, send_sem=send, recv_sem=recv, device_id=device, device_id_type=MESH
    )


class Gather:
    def __init__(self, buf, layers, place, sems):
        self.buf, self.layers, self.place = buf, layers, place
        self.z, self.y, self.x, self.tp = place
        self.rows = buf.shape[0] // (4 * layers)
        self.s_x, self.r_x, self.s_y, self.r_y, self.s_up, self.s_dn, self.r_z = sems

    def at(self, zi, yi, xi, piece=None):
        start = ((zi * 2 + yi) * 2 + xi) * self.rows
        if piece is None:
            return self.buf.at[pl.ds(pl.multiple_of(start, self.rows), self.rows)]
        half = self.rows // 2
        return self.buf.at[pl.ds(pl.multiple_of(start + piece * half, half), half)]

    def device(self, zi, yi, xi):
        return ((zi * 2 + yi) * 2 + xi, self.tp)

    def copy_x(self, zi, j):
        ref = self.at(zi, self.y if j < 2 else 1 - self.y, self.x, (0, 1, 0)[j])
        return remote(ref, ref, self.s_x.at[zi, j], self.r_x.at[zi, j],
                      self.device(self.z, self.y, 1 - self.x))

    def copy_y(self, zi, j):
        ref = self.at(zi, self.y, self.x if j < 2 else 1 - self.x, (1, 0, 1)[j])
        return remote(ref, ref, self.s_y.at[zi, j], self.r_y.at[zi, j],
                      self.device(self.z, 1 - self.y, self.x))

    def copy_z(self, zi, step):
        ref = self.at(zi, self.y, self.x)
        sem = self.s_up if step > 0 else self.s_dn
        return remote(ref, ref, sem.at[zi], self.r_z.at[zi],
                      self.device(self.z + step, self.y, self.x))

    def order(self, t):
        z, last = self.z, self.layers - 1
        near = z - (t + 1) // 2 if t % 2 else z + t // 2
        m = jnp.minimum(z, last - z)
        far = jnp.where(z < last - z, t, last - t)
        return jnp.where(t <= 2 * m, near, far)

    def column(self, t):
        zi = self.order(t)
        if t > 0:
            self.copy_z(zi, 1).wait_recv()
        self.copy_y(zi, 1).start()
        self.copy_x(zi, 1).start()

        @pl.when((zi <= self.z) & (self.z < self.layers - 1))
        def _():
            self.copy_z(zi, 1).start()

        @pl.when((zi >= self.z) & (self.z > 0))
        def _():
            self.copy_z(zi, -1).start()

        self.copy_x(zi, 0).start()
        self.copy_y(zi, 0).start()

    def cross(self, t):
        zi = self.order(t)
        self.copy_y(zi, 1).wait_recv()
        self.copy_x(zi, 2).start()
        self.copy_x(zi, 1).wait_recv()
        self.copy_y(zi, 2).start()

    def arrive(self, t):
        zi = self.order(t)
        for j in (0, 2):
            self.copy_x(zi, j).wait_recv()
            self.copy_y(zi, j).wait_recv()
        return zi

    def drain(self):
        for t in range(self.layers):
            zi = self.order(t)
            for j in range(3):
                self.copy_x(zi, j).wait_send()
                self.copy_y(zi, j).wait_send()

            @pl.when((zi <= self.z) & (self.z < self.layers - 1))
            def _():
                self.copy_z(zi, 1).wait_send()

            @pl.when((zi >= self.z) & (self.z > 0))
            def _():
                self.copy_z(zi, -1).wait_send()


def nt_dot(a, b):
    return lax.dot_general(a, b, (((1,), (1,)), ((), ())), preferred_element_type=F32)


def tn_dot(a, b):
    return lax.dot_general(a, b, (((0,), (0,)), ((), ())), preferred_element_type=F32)


def kernel(layers, peers, tokens, gain, wq, wk, wv, wo, rates, state_init, out_gain, freq, out,
           w_all, wo_all, normed, acc, cosine, sine, q_rot, k_rot, v_row, inner, prev, state,
           hidden, part, landed, own, tot_send, tot_recv, excl, excl_d, z_send, z_recv, incoming,
           local_sem, nrm_s, nrm_r, part_s, part_r, st_s, st_r, zs_s, zs_r, *gather_sems):
    me, tp = lax.axis_index("sp"), lax.axis_index("tp")
    z, y, x = me // 4, (me // 2) % 2, me % 2
    rows_here, width = tokens.shape
    span = rows_here * peers
    cols = wq.shape[1]
    heads = cols // HEAD_DIM
    blocks = span // BLOCK
    shard = wq.shape[0]
    gq = Gather(w_all, layers, (z, y, x, tp), gather_sems[:7])
    go = Gather(wo_all, layers, (z, y, x, tp), gather_sems[7:])

    mine = pl.ds(pl.multiple_of(me * shard, shard), shard)
    fills = [
        pltpu.make_async_copy(src, dst, local_sem.at[i])
        for i, (src, dst) in enumerate((
            (wq, w_all.at[mine, pl.ds(0, cols)]),
            (wk, w_all.at[mine, pl.ds(cols, cols)]),
            (wv, w_all.at[mine, pl.ds(2 * cols, cols)]),
            (wo, wo_all.at[mine]),
        ))
    ]
    for fill in fills:
        fill.start()

    barrier = pltpu.get_barrier_semaphore()

    def greet(device):
        pl.semaphore_signal(barrier, inc=1, device_id=device, device_id_type=MESH)

    greet(gq.device(z, y, 1 - x))
    greet(gq.device(z, 1 - y, x))
    for d in range(1, peers):
        greet((me, (tp + d) % peers))

    @pl.when(z > 0)
    def _():
        greet(gq.device(z - 1, y, x))

    @pl.when(z < layers - 1)
    def _():
        greet(gq.device(z + 1, y, x))

    pl.semaphore_wait(
        barrier, 1 + peers + jnp.minimum(z, 1) + jnp.minimum(layers - 1 - z, 1))

    for fill in fills:
        fill.wait()
    gq.column(0)

    base = pl.multiple_of(tp * rows_here, rows_here)
    tile = 64

    @pl.loop(0, rows_here // tile)
    def _(i):
        at = pl.ds(pl.multiple_of(i * tile, tile), tile)
        u = tokens[at, :].astype(F32)
        scale = lax.rsqrt(jnp.mean(u * u, axis=-1, keepdims=True) + EPS)
        normed[pl.ds(pl.multiple_of(base + i * tile, tile), tile), :] = (
            u * scale * gain[...]
        ).astype(BF16)

    def send_normed(d):
        ref = normed.at[pl.ds(base, rows_here)]
        return remote(ref, ref, nrm_s.at[d - 1], nrm_r.at[d - 1], (me, (tp + d) % peers))

    @pl.loop(0, span // BLOCK)
    def _(i):
        at = pl.ds(pl.multiple_of(i * BLOCK, BLOCK), BLOCK)
        pos = lax.broadcasted_iota(jnp.int32, (BLOCK, HEAD_DIM), 0) + (me * span + i * BLOCK)
        angle = pos.astype(F32) * freq[...]
        lane = lax.broadcasted_iota(jnp.int32, (BLOCK, HEAD_DIM), 1)
        sin = jnp.sin(angle)
        cosine[at, :] = jnp.cos(angle)
        sine[at, :] = jnp.where(lane < HEAD_DIM // 2, -sin, sin)

    for d in range(1, peers):
        send_normed(d).start()
    if layers > 1:
        gq.column(1)
    gq.cross(0)
    for d in range(1, peers):
        send_normed(d).wait_recv()

    deep = 4 * shard
    m_tile = 256

    def product(t):
        zi = gq.arrive(t)
        at_k = pl.ds(pl.multiple_of(zi * deep, deep), deep)

        @pl.loop(0, span // m_tile)
        def _(i):
            at = pl.ds(pl.multiple_of(i * m_tile, m_tile), m_tile)
            for c in range(3):
                at_c = pl.ds(c * cols, cols)
                term = jnp.dot(normed[at, at_k], w_all[at_k, at_c], preferred_element_type=F32)
                acc[at, at_c] = term if t == 0 else acc[at, at_c] + term

    for t in range(layers):
        if t + 2 < layers:
            gq.column(t + 2)
        else:
            go.column(t + 2 - layers)
        if t + 1 < layers:
            gq.cross(t + 1)
        product(t)

    gap = (lax.broadcasted_iota(jnp.int32, (BLOCK, BLOCK), 0)
           - lax.broadcasted_iota(jnp.int32, (BLOCK, BLOCK), 1)).astype(F32)
    row = lax.broadcasted_iota(jnp.int32, (BLOCK, HEAD_DIM), 0).astype(F32)

    for h in range(heads):
        state[h] = jnp.zeros((HEAD_DIM, HEAD_DIM), F32)

    def states(b, sums):
        at = pl.ds(pl.multiple_of(b * BLOCK, BLOCK), BLOCK)
        cos, sin = cosine[at, :], sine[at, :]
        new = []
        for h in range(heads):
            rate = rates[b, h]
            head = pl.ds(h * HEAD_DIM, HEAD_DIM)
            u = acc[at, pl.ds(h * HEAD_DIM, HEAD_DIM)]
            q = (u * cos + pltpu.roll(u, HEAD_DIM // 2, 1) * sin).astype(BF16)
            u = acc[at, pl.ds(cols + h * HEAD_DIM, HEAD_DIM)]
            k = (u * cos + pltpu.roll(u, HEAD_DIM // 2, 1) * sin).astype(BF16)
            v = acc[at, pl.ds(2 * cols + h * HEAD_DIM, HEAD_DIM)].astype(BF16)
            q_rot[at, head] = q
            k_rot[at, head] = k
            v_row[at, head] = v
            tail = jnp.exp(-(BLOCK - 1.0 - row) * rate) * HEAD_DIM ** (-0.5)
            kv = tn_dot((k.astype(F32) * tail).astype(BF16), v)
            now = state[h]
            prev[b, h] = now
            state[h] = jnp.exp(jnp.full((1, HEAD_DIM), -float(BLOCK), F32) * rate) * now + kv
            new.append(sums[h] + rate)
        return tuple(new)

    sums = lax.fori_loop(0, blocks, states, (jnp.float32(0.0),) * heads)

    def decay_of(total):
        return jnp.exp(jnp.full((1, HEAD_DIM), -float(BLOCK), F32) * total)

    def pair(step, h, device):
        return remote(tot_send.at[step, h], tot_recv.at[step, h], st_s.at[step, h],
                      st_r.at[step, h], device)

    x_dev, y_dev = gq.device(z, y, 1 - x), gq.device(z, 1 - y, x)
    up_dev = gq.device(z + 1, y, x)

    def put(step, h, decay, value):
        tot_send[step, h, :HEAD_DIM] = value.astype(BF16)
        tot_send[step, h, HEAD_DIM:] = jnp.broadcast_to(decay, (16, HEAD_DIM)).astype(BF16)

    def take(step, h):
        return (tot_recv[step, h, HEAD_DIM:].astype(F32)[:1], tot_recv[step, h, :HEAD_DIM].astype(F32))

    def both(high, decay, value, other):
        d_in, s_in = other
        late = jnp.where(high, decay, d_in)
        total = late * jnp.where(high, s_in, value) + jnp.where(high, value, s_in)
        return decay * d_in, total

    for h in range(heads):
        put(0, h, decay_of(sums[h]), state[h])
        pair(0, h, x_dev).start()

    def inside(b, carry):
        at = pl.ds(pl.multiple_of(b * BLOCK, BLOCK), BLOCK)
        for h in range(heads):
            rate = rates[b, h]
            head = pl.ds(h * HEAD_DIM, HEAD_DIM)
            fall = jnp.where(gap >= 0.0, jnp.exp(-jnp.maximum(gap, 0.0) * rate), 0.0)
            score = nt_dot(q_rot[at, head], k_rot[at, head]) * (fall * HEAD_DIM ** (-0.5))
            inner[at, head] = jnp.dot(score.astype(BF16), v_row[at, head], preferred_element_type=F32)
        return carry

    third = -(-blocks // 3)
    lax.fori_loop(0, third, inside, 0)
    for h in range(heads):
        pair(0, h, x_dev).wait_recv()
        got = take(0, h)
        excl[h] = jnp.where(x == 1, got[1], 0.0)
        excl_d[h] = jnp.broadcast_to(jnp.where(x == 1, got[0], 1.0), (8, HEAD_DIM))
        decay, value = both(x == 1, decay_of(sums[h]), state[h], got)
        put(1, h, decay, value)
        state[h] = value
        own_decay = jnp.broadcast_to(decay, (8, HEAD_DIM))
        incoming[h, :8] = own_decay
        pair(1, h, y_dev).start()
    lax.fori_loop(third, 2 * third, inside, 0)
    for h in range(heads):
        pair(1, h, y_dev).wait_recv()
        got = take(1, h)
        own_d, own_s = excl_d[h][:1], excl[h]
        excl[h] = jnp.where(y == 1, own_d * got[1] + own_s, own_s)
        excl_d[h] = jnp.broadcast_to(jnp.where(y == 1, own_d * got[0], own_d), (8, HEAD_DIM))
        decay, value = both(y == 1, incoming[h, :8][:1], state[h], got)
        state[h] = value

        def lift(h):
            return remote(z_send.at[h], z_recv.at[h], zs_s.at[h], zs_r.at[h], up_dev)

        @pl.when(z == 0)
        def _():
            incoming[h] = state_init[h]

        @pl.when(z > 0)
        def _():
            lift(h).wait_recv()
            incoming[h] = z_recv[h].astype(F32)

        @pl.when(z < layers - 1)
        def _():
            z_send[h] = (decay * incoming[h] + value).astype(BF16)
            lift(h).start()

        incoming[h] = excl_d[h][:1] * incoming[h] + excl[h]

    lax.fori_loop(2 * third, blocks, inside, 0)

    for t in range(layers):
        if t + 2 < layers:
            go.column(t + 2)
        go.cross(t)

    def finish(b, sums):
        at = pl.ds(pl.multiple_of(b * BLOCK, BLOCK), BLOCK)
        new = []
        for h in range(heads):
            rate = rates[b, h]
            head = pl.ds(h * HEAD_DIM, HEAD_DIM)
            before = prev[b, h] + decay_of(sums[h]) * incoming[h]
            read = jnp.exp(-(row + 1.0) * rate)
            kept = inner[at, head] + read * jnp.dot(
                q_rot[at, head], before.astype(BF16), preferred_element_type=F32)
            kept = kept * lax.rsqrt(jnp.mean(kept * kept, axis=-1, keepdims=True) + EPS)
            hidden[at, head] = (kept * out_gain[:, head]).astype(BF16)
            new.append(sums[h] + rate)
        return tuple(new)

    lax.fori_loop(0, blocks, finish, (jnp.float32(0.0),) * heads)
    for t in range(layers):
        go.arrive(t)

    o_tile = min(128, rows_here)

    def project(start, store):
        @pl.loop(0, rows_here // o_tile)
        def _(i):
            rows = pl.ds(pl.multiple_of(start + i * o_tile, o_tile), o_tile)
            store(pl.ds(pl.multiple_of(i * o_tile, o_tile), o_tile),
                  nt_dot(hidden[rows, :], wo_all[...]).astype(BF16))

    def hand(d):
        return remote(part.at[d - 1], landed.at[d - 1], part_s.at[d - 1], part_r.at[d - 1],
                      (me, (tp + d) % peers))

    for d in range(1, peers):
        def keep(at, value):
            part[d - 1, at, :] = value

        project(((tp + d) % peers) * rows_here, keep)
        hand(d).start()

    def keep_own(at, value):
        own[at, :] = value

    project(base, keep_own)
    for d in range(1, peers):
        hand(d).wait_recv()

    @pl.loop(0, rows_here // tile)
    def _(i):
        at = pl.ds(pl.multiple_of(i * tile, tile), tile)
        total = own[at, :].astype(F32)
        for d in range(1, peers):
            total = total + landed[d - 1, at, :].astype(F32)
        out[at, :] = total.astype(BF16)

    gq.drain()
    go.drain()
    for d in range(1, peers):
        send_normed(d).wait_send()
        hand(d).wait_send()
    for h in range(heads):
        pair(0, h, x_dev).wait_send()
        pair(1, h, y_dev).wait_send()

    @pl.when(z < layers - 1)
    def _():
        for h in range(heads):
            remote(z_send.at[h], z_recv.at[h], zs_s.at[h], zs_r.at[h], up_dev).wait_send()


def shards(tokens, norm_gain, w_query, w_key, w_value, decay_rate, state_init, out_gain, w_out):
    n_sp, peers = lax.axis_size("sp"), lax.axis_size("tp")
    layers = n_sp // 4
    rows_here, width = tokens.shape
    span = rows_here * peers
    cols = w_query.shape[1]
    heads = cols // HEAD_DIM
    blocks = span // BLOCK
    half = HEAD_DIM // 2
    freq = ROPE_BASE ** (-jnp.arange(half, dtype=F32) / half)
    freq = jnp.concatenate([freq, freq])[None]
    vmem = pl.BlockSpec(memory_space=pltpu.VMEM)
    hbm = pl.BlockSpec(memory_space=pl.ANY)
    smem = pl.BlockSpec(memory_space=pltpu.SMEM)
    dma = pltpu.SemaphoreType.DMA
    others = max(peers - 1, 1)
    gather_sems = [dma((layers, 3))] * 4 + [dma((layers,))] * 3
    v = pltpu.VMEM
    return pl.pallas_call(
        functools.partial(kernel, layers, peers),
        out_shape=jax.ShapeDtypeStruct((rows_here, width), BF16),
        in_specs=[vmem, vmem, hbm, hbm, hbm, hbm, smem, vmem, vmem, vmem],
        out_specs=vmem,
        scratch_shapes=[
            v((width, 3 * cols), BF16), v((width, cols), BF16), v((span, width), BF16),
            v((span, 3 * cols), F32), v((span, HEAD_DIM), F32), v((span, HEAD_DIM), F32),
            v((span, cols), BF16), v((span, cols), BF16), v((span, cols), BF16),
            v((span, cols), F32), v((blocks, heads, HEAD_DIM, HEAD_DIM), F32),
            v((heads, HEAD_DIM, HEAD_DIM), F32), v((span, cols), BF16),
            v((others, rows_here, width), BF16), v((others, rows_here, width), BF16),
            v((rows_here, width), BF16),
            v((2, heads, HEAD_DIM + 16, HEAD_DIM), BF16), v((2, heads, HEAD_DIM + 16, HEAD_DIM), BF16),
            v((heads, HEAD_DIM, HEAD_DIM), F32), v((heads, 8, HEAD_DIM), F32),
            v((heads, HEAD_DIM, HEAD_DIM), BF16), v((heads, HEAD_DIM, HEAD_DIM), BF16),
            v((heads, HEAD_DIM, HEAD_DIM), F32),
            dma((4,)), dma((others,)), dma((others,)), dma((others,)), dma((others,)),
            dma((2, heads)), dma((2, heads)), dma((heads,)), dma((heads,)),
        ] + gather_sems * 2,
        compiler_params=pltpu.CompilerParams(
            collective_id=0, has_side_effects=True, vmem_limit_bytes=62 * 1024 * 1024),
    )(tokens, norm_gain[None], w_query, w_key, w_value, w_out.T, decay_rate, state_init,
      out_gain[None], freq)


def solution(mesh):
    in_specs = (
        P(("sp", "tp"), None),
        P(),
        P("sp", "tp"),
        P("sp", "tp"),
        P("sp", "tp"),
        P("sp", "tp"),
        P("tp", None, None),
        P("tp"),
        P("tp", "sp"),
    )
    out_specs = P(("sp", "tp"), None)
    return jax.shard_map(shards, mesh=mesh, in_specs=in_specs, out_specs=out_specs, check_vma=False)
```

```python
import functools

import jax
import jax.numpy as jnp
from jax import lax
from jax.experimental import pallas as pl
from jax.experimental.pallas import tpu as pltpu
from jax.sharding import PartitionSpec as P

HEAD_DIM = 128
BLOCK = 128
EPS = 0.1
ROPE_BASE = 10000.0
MESH = pl.DeviceIdType.MESH
F32 = jnp.float32
BF16 = jnp.bfloat16


def remote(src, dst, send, recv, device):
    return pltpu.make_async_remote_copy(
        src_ref=src, dst_ref=dst, send_sem=send, recv_sem=recv, device_id=device, device_id_type=MESH
    )


class Gather:
    def __init__(self, buf, layers, place, sems):
        self.buf, self.layers, self.place = buf, layers, place
        self.z, self.y, self.x, self.tp = place
        self.rows = buf.shape[0] // (4 * layers)
        self.s_x, self.r_x, self.s_y, self.r_y, self.s_up, self.s_dn, self.r_z = sems

    def at(self, zi, yi, xi, piece=None):
        start = ((zi * 2 + yi) * 2 + xi) * self.rows
        if piece is None:
            return self.buf.at[pl.ds(pl.multiple_of(start, self.rows), self.rows)]
        half = self.rows // 2
        return self.buf.at[pl.ds(pl.multiple_of(start + piece * half, half), half)]

    def device(self, zi, yi, xi):
        return ((zi * 2 + yi) * 2 + xi, self.tp)

    def copy_x(self, zi, j):
        ref = self.at(zi, self.y if j < 2 else 1 - self.y, self.x, (0, 1, 0)[j])
        return remote(ref, ref, self.s_x.at[zi, j], self.r_x.at[zi, j],
                      self.device(self.z, self.y, 1 - self.x))

    def copy_y(self, zi, j):
        ref = self.at(zi, self.y, self.x if j < 2 else 1 - self.x, (1, 0, 1)[j])
        return remote(ref, ref, self.s_y.at[zi, j], self.r_y.at[zi, j],
                      self.device(self.z, 1 - self.y, self.x))

    def copy_z(self, zi, step):
        ref = self.at(zi, self.y, self.x)
        sem = self.s_up if step > 0 else self.s_dn
        return remote(ref, ref, sem.at[zi], self.r_z.at[zi],
                      self.device(self.z + step, self.y, self.x))

    def order(self, t):
        z, last = self.z, self.layers - 1
        near = z - (t + 1) // 2 if t % 2 else z + t // 2
        m = jnp.minimum(z, last - z)
        far = jnp.where(z < last - z, t, last - t)
        return jnp.where(t <= 2 * m, near, far)

    def column(self, t):
        zi = self.order(t)
        if t > 0:
            self.copy_z(zi, 1).wait_recv()
        self.copy_y(zi, 1).start()
        self.copy_x(zi, 1).start()

        @pl.when((zi <= self.z) & (self.z < self.layers - 1))
        def _():
            self.copy_z(zi, 1).start()

        @pl.when((zi >= self.z) & (self.z > 0))
        def _():
            self.copy_z(zi, -1).start()

        self.copy_x(zi, 0).start()
        self.copy_y(zi, 0).start()

    def cross(self, t):
        zi = self.order(t)
        self.copy_y(zi, 1).wait_recv()
        self.copy_x(zi, 2).start()
        self.copy_x(zi, 1).wait_recv()
        self.copy_y(zi, 2).start()

    def arrive(self, t):
        zi = self.order(t)
        for j in (0, 2):
            self.copy_x(zi, j).wait_recv()
            self.copy_y(zi, j).wait_recv()
        return zi

    def drain(self):
        for t in range(self.layers):
            zi = self.order(t)
            for j in range(3):
                self.copy_x(zi, j).wait_send()
                self.copy_y(zi, j).wait_send()

            @pl.when((zi <= self.z) & (self.z < self.layers - 1))
            def _():
                self.copy_z(zi, 1).wait_send()

            @pl.when((zi >= self.z) & (self.z > 0))
            def _():
                self.copy_z(zi, -1).wait_send()


def nt_dot(a, b):
    return lax.dot_general(a, b, (((1,), (1,)), ((), ())), preferred_element_type=F32)


def tn_dot(a, b):
    return lax.dot_general(a, b, (((0,), (0,)), ((), ())), preferred_element_type=F32)


def kernel(layers, peers, tokens, gain, wq, wk, wv, wo, rates, state_init, out_gain, freq, out,
           wkv_all, wq_all, wo_all, normed, acc, cosine, sine, q_rot, k_rot, v_row, inner, prev, state,
           hidden, part, landed, own, tot_send, tot_recv, excl, excl_d, plane_d, z_send, z_recv, incoming,
           local_sem, nrm_s, nrm_r, part_s, part_r, st_s, st_r, zs_s, zs_r, *gather_sems):
    me, tp = lax.axis_index("sp"), lax.axis_index("tp")
    z, y, x = me // 4, (me // 2) % 2, me % 2
    rows_here, width = tokens.shape
    span = rows_here * peers
    cols = wq.shape[1]
    heads = cols // HEAD_DIM
    blocks = span // BLOCK
    shard = wq.shape[0]
    gk = Gather(wkv_all, layers, (z, y, x, tp), gather_sems[:7])
    gq = Gather(wq_all, layers, (z, y, x, tp), gather_sems[7:14])
    go = Gather(wo_all, layers, (z, y, x, tp), gather_sems[14:])

    mine = pl.ds(pl.multiple_of(me * shard, shard), shard)
    fills = [
        pltpu.make_async_copy(src, dst, local_sem.at[i])
        for i, (src, dst) in enumerate((
            (wq, wq_all.at[mine]),
            (wk, wkv_all.at[mine, pl.ds(0, cols)]),
            (wv, wkv_all.at[mine, pl.ds(cols, cols)]),
            (wo, wo_all.at[mine]),
        ))
    ]
    for fill in fills:
        fill.start()

    barrier = pltpu.get_barrier_semaphore()

    def greet(device):
        pl.semaphore_signal(barrier, inc=1, device_id=device, device_id_type=MESH)

    greet(gq.device(z, y, 1 - x))
    greet(gq.device(z, 1 - y, x))
    for d in range(1, peers):
        greet((me, (tp + d) % peers))

    @pl.when(z > 0)
    def _():
        greet(gq.device(z - 1, y, x))

    @pl.when(z < layers - 1)
    def _():
        greet(gq.device(z + 1, y, x))

    pl.semaphore_wait(
        barrier, 1 + peers + jnp.minimum(z, 1) + jnp.minimum(layers - 1 - z, 1))

    for fill in fills:
        fill.wait()
    gk.column(0)

    base = pl.multiple_of(tp * rows_here, rows_here)
    tile = 64

    @pl.loop(0, rows_here // tile)
    def _(i):
        at = pl.ds(pl.multiple_of(i * tile, tile), tile)
        u = tokens[at, :].astype(F32)
        scale = lax.rsqrt(jnp.mean(u * u, axis=-1, keepdims=True) + EPS)
        normed[pl.ds(pl.multiple_of(base + i * tile, tile), tile), :] = (
            u * scale * gain[...]
        ).astype(BF16)

    def send_normed(d):
        ref = normed.at[pl.ds(base, rows_here)]
        return remote(ref, ref, nrm_s.at[d - 1], nrm_r.at[d - 1], (me, (tp + d) % peers))

    def trig(i, carry):
        at = pl.ds(pl.multiple_of(i * BLOCK, BLOCK), BLOCK)
        pos = lax.broadcasted_iota(jnp.int32, (BLOCK, HEAD_DIM), 0) + (me * span + i * BLOCK)
        angle = pos.astype(F32) * freq[...]
        lane = lax.broadcasted_iota(jnp.int32, (BLOCK, HEAD_DIM), 1)
        sin = jnp.sin(angle)
        cosine[at, :] = jnp.cos(angle)
        sine[at, :] = jnp.where(lane < HEAD_DIM // 2, -sin, sin)
        return carry

    for d in range(1, peers):
        send_normed(d).start()
    gk.column(1)
    gk.cross(0)
    if layers > 2:
        gk.column(2)
    for d in range(1, peers):
        send_normed(d).wait_recv()

    deep = 4 * shard
    m_tile = 256

    def product(gather, t, first, count):
        zi = gather.arrive(t)
        at_k = pl.ds(pl.multiple_of(zi * deep, deep), deep)

        @pl.loop(0, span // m_tile)
        def _(i):
            at = pl.ds(pl.multiple_of(i * m_tile, m_tile), m_tile)
            for c in range(count):
                term = jnp.dot(normed[at, at_k], gather.buf[at_k, c * cols:(c + 1) * cols],
                               preferred_element_type=F32)
                at_c = pl.ds((first + c) * cols, cols)
                acc[at, at_c] = term if t == 0 else acc[at, at_c] + term

    cut = [blocks * i // layers for i in range(layers + 1)]
    for t in range(layers):
        lax.fori_loop(cut[t], cut[t + 1], trig, 0)
        if t + 1 < layers:
            gk.cross(t + 1)
        if t + 3 < layers:
            gk.column(t + 3)
        if t == layers - 2:
            gq.column(0)
            gq.column(1)
        product(gk, t, 1, 2)
    gq.cross(0)
    for t in range(2, layers):
        gq.column(t)
        gq.cross(t - 1)

    gap = (lax.broadcasted_iota(jnp.int32, (BLOCK, BLOCK), 0)
           - lax.broadcasted_iota(jnp.int32, (BLOCK, BLOCK), 1)).astype(F32)
    row = lax.broadcasted_iota(jnp.int32, (BLOCK, HEAD_DIM), 0).astype(F32)

    for h in range(heads):
        state[h] = jnp.zeros((HEAD_DIM, HEAD_DIM), F32)

    def states(b, sums):
        at = pl.ds(pl.multiple_of(b * BLOCK, BLOCK), BLOCK)
        cos, sin = cosine[at, :], sine[at, :]
        new = []
        for h in range(heads):
            rate = rates[b, h]
            head = pl.ds(h * HEAD_DIM, HEAD_DIM)
            u = acc[at, pl.ds(cols + h * HEAD_DIM, HEAD_DIM)]
            k = (u * cos + pltpu.roll(u, HEAD_DIM // 2, 1) * sin).astype(BF16)
            v = acc[at, pl.ds(2 * cols + h * HEAD_DIM, HEAD_DIM)].astype(BF16)
            k_rot[at, head] = k
            v_row[at, head] = v
            tail = jnp.exp(-(BLOCK - 1.0 - row) * rate) * HEAD_DIM ** (-0.5)
            kv = tn_dot((k.astype(F32) * tail).astype(BF16), v)
            now = state[h]
            prev[b, h] = now
            state[h] = jnp.exp(jnp.full((1, HEAD_DIM), -float(BLOCK), F32) * rate) * now + kv
            new.append(sums[h] + rate)
        return tuple(new)

    sums = lax.fori_loop(0, blocks, states, (jnp.float32(0.0),) * heads)

    def decay_of(total):
        return jnp.exp(jnp.full((1, HEAD_DIM), -float(BLOCK), F32) * total)

    def pair(step, h, device):
        return remote(tot_send.at[step, h], tot_recv.at[step, h], st_s.at[step, h],
                      st_r.at[step, h], device)

    x_dev, y_dev = gq.device(z, y, 1 - x), gq.device(z, 1 - y, x)
    up_dev = gq.device(z + 1, y, x)

    def put(step, h, decay, value):
        tot_send[step, h, :HEAD_DIM] = value.astype(BF16)
        tot_send[step, h, HEAD_DIM:] = jnp.broadcast_to(decay, (16, HEAD_DIM)).astype(BF16)

    def take(step, h):
        return (tot_recv[step, h, HEAD_DIM:].astype(F32)[:1], tot_recv[step, h, :HEAD_DIM].astype(F32))

    def both(high, decay, value, other):
        d_in, s_in = other
        late = jnp.where(high, decay, d_in)
        total = late * jnp.where(high, s_in, value) + jnp.where(high, value, s_in)
        return decay * d_in, total

    for h in range(heads):
        put(0, h, decay_of(sums[h]), state[h])
        pair(0, h, x_dev).start()

    def inside(b, carry):
        at = pl.ds(pl.multiple_of(b * BLOCK, BLOCK), BLOCK)
        cos, sin = cosine[at, :], sine[at, :]
        for h in range(heads):
            rate = rates[b, h]
            head = pl.ds(h * HEAD_DIM, HEAD_DIM)
            u = acc[at, head]
            q_rot[at, head] = (u * cos + pltpu.roll(u, HEAD_DIM // 2, 1) * sin).astype(BF16)
            fall = jnp.where(gap >= 0.0, jnp.exp(-jnp.maximum(gap, 0.0) * rate), 0.0)
            score = nt_dot(q_rot[at, head], k_rot[at, head]) * (fall * HEAD_DIM ** (-0.5))
            inner[at, head] = jnp.dot(score.astype(BF16), v_row[at, head], preferred_element_type=F32)
        return carry

    gq.cross(layers - 1)
    go.column(0)
    for t in range(layers // 2):
        product(gq, t, 0, 1)
    for h in range(heads):
        pair(0, h, x_dev).wait_recv()
        got = take(0, h)
        excl[h] = jnp.where(x == 1, got[1], 0.0)
        excl_d[h] = jnp.broadcast_to(jnp.where(x == 1, got[0], 1.0), (8, HEAD_DIM))
        decay, value = both(x == 1, decay_of(sums[h]), state[h], got)
        put(1, h, decay, value)
        state[h] = value
        own_decay = jnp.broadcast_to(decay, (8, HEAD_DIM))
        incoming[h, :8] = own_decay
        pair(1, h, y_dev).start()
    go.column(1)
    go.cross(0)
    for t in range(layers // 2, layers):
        product(gq, t, 0, 1)
    for h in range(heads):
        pair(1, h, y_dev).wait_recv()
        got = take(1, h)
        own_d, own_s = excl_d[h][:1], excl[h]
        excl[h] = jnp.where(y == 1, own_d * got[1] + own_s, own_s)
        excl_d[h] = jnp.broadcast_to(jnp.where(y == 1, own_d * got[0], own_d), (8, HEAD_DIM))
        decay, value = both(y == 1, incoming[h, :8][:1], state[h], got)
        state[h] = value
        plane_d[h] = jnp.broadcast_to(decay, (8, HEAD_DIM))

    def lift(h):
        return remote(z_send.at[h], z_recv.at[h], zs_s.at[h], zs_r.at[h], up_dev)

    def relay(from_below):
        for h in range(heads):
            if from_below:
                lift(h).wait_recv()
                incoming[h] = z_recv[h].astype(F32)
            else:
                incoming[h] = state_init[h]

            @pl.when(z < layers - 1)
            def _():
                z_send[h] = (plane_d[h][:1] * incoming[h] + state[h]).astype(BF16)
                lift(h).start()

            incoming[h] = excl_d[h][:1] * incoming[h] + excl[h]

    pl.when(z == 0)(lambda: relay(False))
    if layers > 2:
        go.column(2)
        go.cross(1)
    third = -(-blocks // 3)
    lax.fori_loop(0, third, inside, 0)
    pl.when(z == 1)(lambda: relay(True))
    for t in range(3, layers):
        go.column(t)
        go.cross(t - 1)
    lax.fori_loop(third, 2 * third, inside, 0)
    pl.when(z == 2)(lambda: relay(True))
    go.cross(layers - 1)
    lax.fori_loop(2 * third, blocks, inside, 0)
    pl.when(z > 2)(lambda: relay(True))

    def finish(b, sums):
        at = pl.ds(pl.multiple_of(b * BLOCK, BLOCK), BLOCK)
        new = []
        for h in range(heads):
            rate = rates[b, h]
            head = pl.ds(h * HEAD_DIM, HEAD_DIM)
            before = prev[b, h] + decay_of(sums[h]) * incoming[h]
            read = jnp.exp(-(row + 1.0) * rate)
            kept = inner[at, head] + read * jnp.dot(
                q_rot[at, head], before.astype(BF16), preferred_element_type=F32)
            kept = kept * lax.rsqrt(jnp.mean(kept * kept, axis=-1, keepdims=True) + EPS)
            hidden[at, head] = (kept * out_gain[:, head]).astype(BF16)
            new.append(sums[h] + rate)
        return tuple(new)

    lax.fori_loop(0, blocks, finish, (jnp.float32(0.0),) * heads)
    for t in range(layers):
        go.arrive(t)

    o_tile = min(128, rows_here)

    def project(start, store):
        @pl.loop(0, rows_here // o_tile)
        def _(i):
            rows = pl.ds(pl.multiple_of(start + i * o_tile, o_tile), o_tile)
            store(pl.ds(pl.multiple_of(i * o_tile, o_tile), o_tile),
                  nt_dot(hidden[rows, :], wo_all[...]).astype(BF16))

    def hand(d):
        return remote(part.at[d - 1], landed.at[d - 1], part_s.at[d - 1], part_r.at[d - 1],
                      (me, (tp + d) % peers))

    for d in range(1, peers):
        def keep(at, value):
            part[d - 1, at, :] = value

        project(((tp + d) % peers) * rows_here, keep)
        hand(d).start()

    def keep_own(at, value):
        own[at, :] = value

    project(base, keep_own)
    for d in range(1, peers):
        hand(d).wait_recv()

    @pl.loop(0, rows_here // tile)
    def _(i):
        at = pl.ds(pl.multiple_of(i * tile, tile), tile)
        total = own[at, :].astype(F32)
        for d in range(1, peers):
            total = total + landed[d - 1, at, :].astype(F32)
        out[at, :] = total.astype(BF16)

    gk.drain()
    gq.drain()
    go.drain()
    for d in range(1, peers):
        send_normed(d).wait_send()
        hand(d).wait_send()
    for h in range(heads):
        pair(0, h, x_dev).wait_send()
        pair(1, h, y_dev).wait_send()

    @pl.when(z < layers - 1)
    def _():
        for h in range(heads):
            remote(z_send.at[h], z_recv.at[h], zs_s.at[h], zs_r.at[h], up_dev).wait_send()


def shards(tokens, norm_gain, w_query, w_key, w_value, decay_rate, state_init, out_gain, w_out):
    n_sp, peers = lax.axis_size("sp"), lax.axis_size("tp")
    layers = n_sp // 4
    rows_here, width = tokens.shape
    span = rows_here * peers
    cols = w_query.shape[1]
    heads = cols // HEAD_DIM
    blocks = span // BLOCK
    half = HEAD_DIM // 2
    freq = ROPE_BASE ** (-jnp.arange(half, dtype=F32) / half)
    freq = jnp.concatenate([freq, freq])[None]
    vmem = pl.BlockSpec(memory_space=pltpu.VMEM)
    hbm = pl.BlockSpec(memory_space=pl.ANY)
    smem = pl.BlockSpec(memory_space=pltpu.SMEM)
    dma = pltpu.SemaphoreType.DMA
    others = max(peers - 1, 1)
    gather_sems = [dma((layers, 3))] * 4 + [dma((layers,))] * 3
    v = pltpu.VMEM
    return pl.pallas_call(
        functools.partial(kernel, layers, peers),
        out_shape=jax.ShapeDtypeStruct((rows_here, width), BF16),
        in_specs=[vmem, vmem, hbm, hbm, hbm, hbm, smem, vmem, vmem, vmem],
        out_specs=vmem,
        scratch_shapes=[
            v((width, 2 * cols), BF16), v((width, cols), BF16), v((width, cols), BF16),
            v((span, width), BF16),
            v((span, 3 * cols), F32), v((span, HEAD_DIM), F32), v((span, HEAD_DIM), F32),
            v((span, cols), BF16), v((span, cols), BF16), v((span, cols), BF16),
            v((span, cols), F32), v((blocks, heads, HEAD_DIM, HEAD_DIM), F32),
            v((heads, HEAD_DIM, HEAD_DIM), F32), v((span, cols), BF16),
            v((others, rows_here, width), BF16), v((others, rows_here, width), BF16),
            v((rows_here, width), BF16),
            v((2, heads, HEAD_DIM + 16, HEAD_DIM), BF16), v((2, heads, HEAD_DIM + 16, HEAD_DIM), BF16),
            v((heads, HEAD_DIM, HEAD_DIM), F32), v((heads, 8, HEAD_DIM), F32),
            v((heads, 8, HEAD_DIM), F32),
            v((heads, HEAD_DIM, HEAD_DIM), BF16), v((heads, HEAD_DIM, HEAD_DIM), BF16),
            v((heads, HEAD_DIM, HEAD_DIM), F32),
            dma((4,)), dma((others,)), dma((others,)), dma((others,)), dma((others,)),
            dma((2, heads)), dma((2, heads)), dma((heads,)), dma((heads,)),
        ] + gather_sems * 3,
        compiler_params=pltpu.CompilerParams(
            collective_id=0, has_side_effects=True, vmem_limit_bytes=62 * 1024 * 1024),
    )(tokens, norm_gain[None], w_query, w_key, w_value, w_out.T, decay_rate, state_init,
      out_gain[None], freq)


def solution(mesh):
    in_specs = (
        P(("sp", "tp"), None),
        P(),
        P("sp", "tp"),
        P("sp", "tp"),
        P("sp", "tp"),
        P("sp", "tp"),
        P("tp", None, None),
        P("tp"),
        P("tp", "sp"),
    )
    out_specs = P(("sp", "tp"), None)
    return jax.shard_map(shards, mesh=mesh, in_specs=in_specs, out_specs=out_specs, check_vma=False)
```
